32 devices in a mesh: sp: 8 (over z, x), tp: 4 (over y, core).
Axes of the slice: x: 2, y: 2, z: 4, core: 2. Of those that a mesh axis runs over, the one named last changes fastest.
Arguments:
- queries: bfloat16 [4096, 2048], P('sp', 'tp'), may hold values from -4.5 to 4.5
- keys: bfloat16 [4096, 2048], P('sp', 'tp'), may hold values from -4.5 to 4.5
- values: bfloat16 [4096, 2048], P('sp', 'tp'), may hold values from -6 to 6
- forget_logits: float32 [4096, 16], P('sp', 'tp'), may hold values from -1 to 20
- layer_input: bfloat16 [4096, 4096], P('sp', 'tp'), may hold values from -0.125 to 0.125
- out_grad: bfloat16 [4096, 2048], P('sp', 'tp'), may hold values from -6 to 6
Outputs:
- query_grad: float32 [4096, 2048], P('sp', 'tp')
- key_grad: float32 [4096, 2048], P('sp', 'tp')
- value_grad: float32 [4096, 2048], P('sp', 'tp')
- weight_grad: float32 [4096, 2048], P('sp', 'tp')
The draws below stay inside these ranges and needn't reach their ends.
All inputs are finite; a program needn't handle non-finite values.
Results may differ from the reference program's by a relative error of at most 0.04.
Values may be sent and summed in bfloat16 or wider, within the bound.
A program may use at most 64 MiB of HBM per device.

```python
import math
import jax
import jax.numpy as jnp
from jax import lax

DMODEL = 4096
HEADS = 16
HEAD = 128
TOK_DEV = 512
TOKENS = 4096


def drawn_pair(key):
    full_shape = (TOKENS, HEADS * HEAD)
    query_rows = jnp.clip(jax.random.normal(jax.random.fold_in(key, 101), full_shape, jnp.float32), -4.5, 4.5)
    key_rows = jnp.clip(jax.random.normal(jax.random.fold_in(key, 102), full_shape, jnp.float32), -4.5, 4.5)
    return (query_rows, key_rows)


def draw_queries(key, part):
    return drawn_pair(key)[0].astype(jnp.bfloat16)


def draw_keys(key, part):
    return drawn_pair(key)[1].astype(jnp.bfloat16)


def draw_forget_logits(key, part):
    ranks = jax.random.permutation(jax.random.fold_in(key, 201), HEADS)
    quick = ranks < HEADS // 2
    levels = jax.random.uniform(jax.random.fold_in(key, 202), (HEADS,), jnp.float32, -0.5, 0.5)
    base_level = jnp.where(quick, math.log(80.0), math.log(TOKENS) + 1.0) + levels
    span_rows = max(TOK_DEV // 2, 1)
    shifts = jax.random.uniform(jax.random.fold_in(key, 203), (TOKENS // span_rows + 1, 1), jnp.float32, -0.9, 0.9)
    span_shift = jnp.repeat(shifts, span_rows, axis=0)[:TOKENS]
    noise = jnp.clip(jax.random.normal(jax.random.fold_in(key, 204), (TOKENS, HEADS), jnp.float32), -3.0, 3.0)
    return base_level[None, :] + span_shift + noise


def raised(values, own_key, source, target, parts, factor):
    def block_of(position):
        return (jnp.arange(values.shape[position]) // (values.shape[position] // parts)).reshape((-1,) + (1,) * (values.ndim - 1 - position))

    one_side = jax.random.permutation(own_key, parts)[block_of(target)]
    other_side = (block_of(target) + parts // 2) % parts
    return jnp.where((block_of(source) == one_side) | (block_of(source) == other_side), factor * values, values)


def level_of(key, shape, cuts, smallest, top_value):
    factor_of = 1.0
    for axis_at, shards_of in cuts:
        heights = jax.random.uniform(jax.random.fold_in(jax.random.fold_in(key, 6), axis_at), (shards_of,), jnp.float32, smallest / len(cuts), top_value / len(cuts))
        factor_of = factor_of * jnp.repeat(jnp.exp(heights), shape[axis_at] // shards_of).reshape((-1,) + (1,) * (len(shape) - 1 - axis_at))
    return factor_of


def gaussian(own_key, extent, spread, bound, cuts=(), kind=jnp.bfloat16):
    drawn = spread * jax.random.normal(own_key, extent, jnp.float32)
    if cuts:
        drawn = drawn * level_of(own_key, extent, cuts, -0.22, 0.18)
    return jnp.clip(drawn, -bound, bound).astype(kind)


def heavy_noise(key, extent, width, reach, pieces, heavy, kind=jnp.bfloat16):
    entries = width * jax.random.normal(key, extent, jnp.float32)
    if pieces:
        entries = entries * level_of(key, extent, pieces, -0.22, 0.18)
    return jnp.clip(raised(entries, jax.random.fold_in(key, 3), *heavy), -reach, reach).astype(kind)


def setup_inputs(seed: int = 0) -> dict:
    key_list = jax.random.split(jax.random.key(seed), 7)
    return {
        "queries": draw_queries(jax.random.fold_in(key_list[6], 71), 0),
        "keys": draw_keys(jax.random.fold_in(key_list[6], 71), 0),
        "values": gaussian(key_list[2], (TOKENS, HEADS * HEAD), 1.0, 6.0, ((0, 8), (1, 4))),
        "forget_logits": draw_forget_logits(jax.random.fold_in(key_list[6], 71), 0),
        "layer_input": heavy_noise(key_list[4], (TOKENS, DMODEL), TOKENS ** -0.5, 0.125, ((0, 8), (1, 4)), (0, 1, 8, 2.0)),
        "out_grad": heavy_noise(key_list[5], (TOKENS, HEADS * HEAD), 1.0, 6.0, ((0, 8), (1, 4)), (0, 1, 8, 2.0)),
    }


def query_block(row_count):
    block_size = row_count
    while block_size > 512 and block_size % 2 == 0:
        block_size //= 2
    return block_size


def reference(queries, keys, values, forget_logits, layer_input, out_grad):
    row_count = queries.shape[0]
    head_total = queries.shape[1] // HEAD
    score_scale = HEAD ** -0.5
    gate_sums = jnp.cumsum(jax.nn.log_sigmoid(forget_logits), axis=0)
    positions = jnp.arange(row_count, dtype=jnp.int32)
    block_size = query_block(row_count)
    block_count = row_count // block_size

    def by_head(array):
        return array.reshape(row_count, head_total, HEAD).transpose(1, 0, 2)

    def one_head(inputs):
        head_query, head_key, head_value, head_grad, head_gates = inputs

        def one_block(carry, number):
            key_total, value_total = carry
            begin_at = number * block_size
            query_rows = lax.dynamic_slice_in_dim(head_query, begin_at, block_size, 0)
            grad_rows = lax.dynamic_slice_in_dim(head_grad, begin_at, block_size, 0)
            gate_rows = lax.dynamic_slice_in_dim(head_gates, begin_at, block_size, 0)
            scores = jnp.dot(query_rows, head_key.T, preferred_element_type=jnp.float32) * score_scale
            scores = scores + gate_rows[:, None] - head_gates[None, :]
            query_pos = begin_at + jnp.arange(block_size, dtype=jnp.int32)
            visible = positions[None, :] <= query_pos[:, None]
            row_max = jnp.max(jnp.where(visible, scores, -1.0e30), axis=1)
            weights = jnp.where(visible, jnp.exp(scores - row_max[:, None]), 0.0)
            weight_sum = jnp.sum(weights, axis=1)
            mixed = jnp.dot(weights.astype(jnp.bfloat16), head_value, preferred_element_type=jnp.float32)
            attended = (mixed / weight_sum[:, None]).astype(jnp.bfloat16)
            log_sums = row_max + jnp.log(weight_sum)
            row_terms = jnp.sum(attended.astype(jnp.float32) * grad_rows.astype(jnp.float32), axis=1)
            probs = jnp.where(visible, jnp.exp(scores - log_sums[:, None]), 0.0)
            prob_grads = jnp.dot(grad_rows, head_value.T, preferred_element_type=jnp.float32)
            score_grads = (probs * (prob_grads - row_terms[:, None])).astype(jnp.bfloat16)
            query_part = score_scale * jnp.dot(score_grads, head_key, preferred_element_type=jnp.float32)
            key_total = key_total + score_scale * jnp.dot(score_grads.T, query_rows, preferred_element_type=jnp.float32)
            value_total = value_total + jnp.dot(probs.astype(jnp.bfloat16).T, grad_rows, preferred_element_type=jnp.float32)
            return (key_total, value_total), query_part

        zeros_head = jnp.zeros((row_count, HEAD), jnp.float32)
        (key_total, value_total), query_parts = lax.scan(one_block, (zeros_head, zeros_head), jnp.arange(block_count, dtype=jnp.int32))
        return query_parts.reshape(row_count, HEAD), key_total, value_total

    query_heads, key_heads, value_heads = lax.map(one_head, (by_head(queries), by_head(keys), by_head(values), by_head(out_grad), gate_sums.T))

    def back_rows(array):
        return array.transpose(1, 0, 2).reshape(row_count, head_total * HEAD)

    query_grad = back_rows(query_heads)
    weight_grad = jnp.dot(layer_input.T, query_grad.astype(jnp.bfloat16), preferred_element_type=jnp.float32)
    return query_grad, back_rows(key_heads), back_rows(value_heads), weight_grad
```

```python
import jax
import jax.numpy as jnp
from jax import lax
from jax.experimental import pallas as pl
from jax.experimental.pallas import tpu as pltpu
from jax.sharding import PartitionSpec as P

HEAD = 128
LOG2E = 1.4426950408889634
SCALE = HEAD ** (-0.5)


def nt(a, b):
    return lax.dot_general(a, b, (((1,), (1,)), ((), ())), preferred_element_type=jnp.float32)


def nn(a, b):
    return lax.dot_general(a, b, (((1,), (0,)), ((), ())), preferred_element_type=jnp.float32)


def attention_kernel(parts, q_ref, g_ref, k_ref, v_ref, gate_ref, dq_ref, dk_ref, dv_ref, kt, vt, sc, dk, dv):
    blocks, rows, _ = k_ref.shape
    sub = q_ref.shape[1]
    part = lax.rem(lax.axis_index("sp"), parts)

    @pl.loop(0, blocks)
    def _(j):
        kt[j] = k_ref[j].T
        vt[j] = v_ref[j].T
        dk[j] = jnp.zeros((rows, HEAD), jnp.float32)
        dv[j] = jnp.zeros((rows, HEAD), jnp.float32)

    @pl.loop(0, blocks)
    def _(b):
        q = q_ref[b]
        g = g_ref[b]
        offset = lax.rem(part + b, parts) * sub

        def score(j):
            return nt(k_ref[j], q) * (SCALE * LOG2E) - gate_ref[j]

        def pass_a(j, top):
            s = score(j)
            sc[j] = s
            return jnp.maximum(top, jnp.max(s, axis=0, keepdims=True))

        top = lax.fori_loop(0, b, pass_a, jnp.full((1, sub), -1e30, jnp.float32))
        key_pos = lax.broadcasted_iota(jnp.int32, (rows, sub), 0)
        query_pos = lax.broadcasted_iota(jnp.int32, (rows, sub), 1) + offset
        s = jnp.where(key_pos <= query_pos, score(b), -1e30)
        sc[b] = s
        top = jnp.maximum(top, jnp.max(s, axis=0, keepdims=True))

        def pass_b(j, state):
            total, mixed = state
            w = jnp.exp2(sc[j] - top)
            sc[j] = w
            total = total + jnp.sum(w, axis=0, keepdims=True)
            return total, mixed + nn(vt[j], w.astype(jnp.bfloat16))

        total, mixed = lax.fori_loop(
            0, b + 1, pass_b, (jnp.zeros((1, sub), jnp.float32), jnp.zeros((HEAD, sub), jnp.float32))
        )
        attended = (mixed / total).astype(jnp.bfloat16).astype(jnp.float32)
        terms = jnp.sum(attended * g.astype(jnp.float32).T, axis=0, keepdims=True)
        inverse = 1.0 / total

        def pass_c(j, acc):
            prob = sc[j] * inverse
            ds = (prob * (nt(v_ref[j], g) - terms)).astype(jnp.bfloat16)
            dv[j] += nn(prob.astype(jnp.bfloat16), g)
            dk[j] += nn(ds, q)
            return acc + nn(kt[j], ds)

        acc = lax.fori_loop(0, b + 1, pass_c, jnp.zeros((HEAD, sub), jnp.float32))
        dq_ref[b] = (acc * SCALE).T.astype(jnp.bfloat16)

    @pl.loop(0, blocks)
    def _(j):
        dk_ref[j] = (dk[j] * SCALE).astype(jnp.bfloat16)
        dv_ref[j] = dv[j].astype(jnp.bfloat16)


def attention(parts, q, g, k, v, gate):
    blocks, rows, _ = k.shape
    sub = q.shape[1]
    vmem = pl.BlockSpec(memory_space=pltpu.VMEM)
    low = jnp.bfloat16
    return pl.pallas_call(
        lambda *refs: attention_kernel(parts, *refs),
        out_shape=(
            jax.ShapeDtypeStruct((blocks, sub, HEAD), low),
            jax.ShapeDtypeStruct((blocks, rows, HEAD), low),
            jax.ShapeDtypeStruct((blocks, rows, HEAD), low),
        ),
        in_specs=[vmem] * 5,
        out_specs=(vmem,) * 3,
        scratch_shapes=[
            pltpu.VMEM((blocks, HEAD, rows), low),
            pltpu.VMEM((blocks, HEAD, rows), low),
            pltpu.VMEM((blocks, rows, sub), jnp.float32),
            pltpu.VMEM((blocks, rows, HEAD), jnp.float32),
            pltpu.VMEM((blocks, rows, HEAD), jnp.float32),
        ],
        compiler_params=pltpu.CompilerParams(vmem_limit_bytes=60 * 1024 * 1024),
        cost_estimate=pl.CostEstimate(
            flops=6 * blocks * blocks * rows * sub * HEAD, bytes_accessed=1 << 22, transcendentals=0
        ),
        name="attention",
    )(q, g, k, v, gate)


def local(queries, keys, values, forget_logits, layer_input, out_grad):
    rows = queries.shape[0]
    heads = queries.shape[1] // HEAD
    shards = lax.axis_size("sp")
    parts = shards // heads
    sub = rows // parts
    me = lax.axis_index("sp")
    head = me // parts
    part = me % parts

    input_whole = lax.all_gather(layer_input, "tp", axis=1, tiled=True)

    local_gates = jnp.cumsum(jax.nn.log_sigmoid(forget_logits), axis=0)
    per_shard = lax.all_gather(local_gates, "sp", axis=0)
    totals = per_shard[:, -1, :]
    before = jnp.cumsum(totals, axis=0) - totals
    sums = per_shard + before[:, None, :]
    gate = lax.dynamic_slice_in_dim(sums, head, 1, 2) * LOG2E

    def whole(a):
        a = a.reshape(rows, heads, HEAD).transpose(1, 0, 2)
        return jnp.broadcast_to(a[:, None], (heads, parts, rows, HEAD)).reshape(shards, rows, HEAD)

    def split(a):
        a = a.reshape(parts, sub, heads, HEAD).transpose(2, 0, 1, 3)
        twice = jnp.concatenate([a, a], axis=1)
        return lax.dynamic_slice_in_dim(twice, me % parts, parts, 1).reshape(shards, sub, HEAD)

    packed = jnp.concatenate([whole(keys), whole(values), split(queries), split(out_grad)], axis=1)
    got = lax.all_to_all(packed, "sp", 0, 0)
    k, v = got[:, :rows], got[:, rows : 2 * rows]
    q, g = got[:, 2 * rows : 2 * rows + sub], got[:, 2 * rows + sub :]
    dq, dk, dv = attention(parts, q, g, k, v, gate)

    back = lax.all_to_all(dq, "sp", 0, 0).reshape(heads, parts, sub, HEAD)
    twice = jnp.concatenate([back, back], axis=1)
    back = lax.dynamic_slice_in_dim(twice, parts - me % parts, parts, 1)
    low = back.transpose(1, 2, 0, 3).reshape(rows, heads * HEAD)
    weight_term = lax.dot_general(
        input_whole, low, (((0,), (0,)), ((), ())), preferred_element_type=jnp.float32
    )
    weight_grad = lax.psum_scatter(
        weight_term.astype(jnp.bfloat16), "sp", scatter_dimension=0, tiled=True
    ).astype(jnp.float32)
    both = lax.all_to_all(jnp.concatenate([dk, dv], axis=1), "sp", 0, 0)
    both = both.reshape(heads, parts, 2, rows, HEAD).astype(jnp.float32).sum(axis=1)
    both = both.transpose(1, 2, 0, 3).reshape(2, rows, heads * HEAD)
    return low.astype(jnp.float32), both[0], both[1], weight_grad


def solution(mesh):
    spec = P("sp", "tp")
    return jax.shard_map(
        local, mesh=mesh, in_specs=(spec,) * 6, out_specs=(spec,) * 4, check_vma=False
    )
```

```python
import jax
import jax.numpy as jnp
from jax import lax
from jax.experimental import pallas as pl
from jax.experimental.pallas import tpu as pltpu
from jax.sharding import PartitionSpec as P

HEAD = 128
LOG2E = 1.4426950408889634
SCALE = HEAD ** (-0.5)
LOW = jnp.bfloat16


def nt(a, b):
    return lax.dot_general(a, b, (((1,), (1,)), ((), ())), preferred_element_type=jnp.float32)


def nn(a, b):
    return lax.dot_general(a, b, (((1,), (0,)), ((), ())), preferred_element_type=jnp.float32)


def kernel_body(
    heads, parts,
    q_in, g_in, k_in, v_in, gate_in,
    dq_out, low_out, dk_out, dv_out,
    kv, qg, gates, kt, vt, bias, sc, dk, dv, dq_stage, part_stage, red, fin, dq_got, kv_got,
    kv_recv, qg_recv, gate_recv, kv_send, qg_send, gate_send, relay_send,
    dq_send, dq_recv, part_send, red_recv, fin_send, fin_recv, local_sem,
):
    blocks, _, rows, _ = kv.shape
    sub = qg.shape[2]
    per_part = blocks // parts
    me = lax.axis_index("sp")
    head = me // parts
    part = lax.rem(me, parts)

    def remote(src, dst, send, recv, target):
        return pltpu.make_async_remote_copy(
            src_ref=src, dst_ref=dst, send_sem=send, recv_sem=recv, device_id={"sp": target}
        )

    barrier = pltpu.get_barrier_semaphore()
    for r in range(1, blocks):
        pl.semaphore_signal(barrier, inc=1, device_id={"sp": lax.rem(me + r, blocks)})
    pl.semaphore_wait(barrier, blocks - 1)

    def lanes(h):
        return pl.ds(pl.multiple_of(h * HEAD, HEAD), HEAD)

    sources = ((k_in, v_in), (q_in, g_in))

    def place(r, c):
        return lax.rem(head + r, heads), lax.rem(part + c, parts)

    def kv_copy(r, i):
        h, _ = place(r, 0)
        return remote(
            sources[0][i].at[:, lanes(h)], kv.at[me, i], kv_send.at[r, i], kv_recv.at[me, i], h * parts + part
        )

    def relay_copy(r, c, i):
        h, other = place(r, c)
        j = h * parts + part
        src = sources[0][i].at[:, lanes(head)] if r == 0 else kv.at[j, i]
        return remote(src, kv.at[j, i], relay_send.at[r, c, i], kv_recv.at[j, i], head * parts + other)

    def q_source(r, c, i):
        h, other = place(r, c)
        begin = pl.multiple_of(lax.rem(other + me, parts) * sub, sub)
        return sources[1][i].at[pl.ds(begin, sub), lanes(h)]

    def q_copy(r, c, i):
        h, other = place(r, c)
        return remote(
            q_source(r, c, i), qg.at[me, i], qg_send.at[r, c, i], qg_recv.at[me, i], h * parts + other
        )

    def gate_copy(r, c):
        h, other = place(r, c)
        return remote(gate_in.at[h], gates.at[me], gate_send.at[r, c], gate_recv.at[me], h * parts + other)

    pairs = [(r, c) for r in range(heads) for c in range(parts) if (r, c) != (0, 0)]
    for r in range(1, heads):
        for i in range(2):
            kv_copy(r, i).start()
    for c in range(1, parts):
        for i in range(2):
            relay_copy(0, c, i).start()
    for r, c in pairs:
        gate_copy(r, c).start()
        for i in range(2):
            q_copy(r, c, i).start()
    own = [
        pltpu.make_async_copy(sources[0][i].at[:, lanes(head)], kv.at[me, i], local_sem.at[i]) for i in range(2)
    ]
    own += [pltpu.make_async_copy(q_source(0, 0, i), qg.at[me, i], local_sem.at[2 + i]) for i in range(2)]
    own += [pltpu.make_async_copy(gate_in.at[head], gates.at[me], local_sem.at[4])]
    for copy in own:
        copy.start()

    def kv_wait(j):
        for i in range(2):
            remote(kv.at[j, i], kv.at[j, i], kv_send.at[0, i], kv_recv.at[j, i], me).wait_recv()

    for r in range(1, heads):
        j = place(r, 0)[0] * parts + part
        kv_wait(j)
        for c in range(1, parts):
            for i in range(2):
                relay_copy(r, c, i).start()
    for copy in own:
        copy.wait()
    for r, c in pairs:
        h, other = place(r, c)
        j = h * parts + other
        if c:
            kv_wait(j)
        for i in range(2):
            remote(qg.at[j, i], qg.at[j, i], qg_send.at[0, 0, i], qg_recv.at[j, i], me).wait_recv()
        remote(gates.at[j], gates.at[j], gate_send.at[0, 0], gate_recv.at[j], me).wait_recv()

    def prepare(j, base):
        kt[j] = kv[j, 0].T
        vt[j] = kv[j, 1].T
        row = gates[j, 0:1] + base
        bias[j] = jnp.broadcast_to(row, (HEAD, rows)).T
        dk[j] = jnp.zeros((rows, HEAD), jnp.float32)
        dv[j] = jnp.zeros((rows, HEAD), jnp.float32)
        return base + gates[j, 1:2]

    lax.fori_loop(0, blocks, prepare, jnp.zeros((1, rows), jnp.float32))

    def compute(b):
        q = qg[b, 0]
        g = qg[b, 1]
        offset = lax.rem(part + b, parts) * sub

        def score(j):
            return nt(kv[j, 0], q) * (SCALE * LOG2E) - bias[j][:, 0:1]

        def pass_a(j, top):
            s = score(j)
            sc[j] = s
            return jnp.maximum(top, jnp.max(s, axis=0, keepdims=True))

        top = lax.fori_loop(0, b, pass_a, jnp.full((1, sub), -1e30, jnp.float32))
        key_pos = lax.broadcasted_iota(jnp.int32, (rows, sub), 0)
        query_pos = lax.broadcasted_iota(jnp.int32, (rows, sub), 1) + offset
        s = jnp.where(key_pos <= query_pos, score(b), -1e30)
        sc[b] = s
        top = jnp.maximum(top, jnp.max(s, axis=0, keepdims=True))

        def pass_b(j, state):
            total, mixed = state
            w = jnp.exp2(sc[j] - top)
            sc[j] = w
            total = total + jnp.sum(w, axis=0, keepdims=True)
            return total, mixed + nn(vt[j], w.astype(LOW))

        total, mixed = lax.fori_loop(
            0, b + 1, pass_b, (jnp.zeros((1, sub), jnp.float32), jnp.zeros((HEAD, sub), jnp.float32))
        )
        attended = (mixed / total).astype(LOW).astype(jnp.float32)
        terms = jnp.sum(attended * g.astype(jnp.float32).T, axis=0, keepdims=True)
        inverse = 1.0 / total

        def pass_c(j, acc):
            prob = sc[j] * inverse
            ds = (prob * (nt(kv[j, 1], g) - terms)).astype(LOW)
            dv[j] += nn(prob.astype(LOW), g)
            dk[j] += nn(ds, q)
            return acc + nn(kt[j], ds)

        acc = lax.fori_loop(0, b + 1, pass_c, jnp.zeros((HEAD, sub), jnp.float32))
        dq_stage[b] = (acc * SCALE).T.astype(LOW)
        part_stage[b, 0] = (dk[b] * SCALE).astype(LOW)
        part_stage[b, 1] = dv[b].astype(LOW)

    def dq_copy(b):
        return remote(
            dq_stage.at[b], dq_got.at[head, lax.rem(part + b, parts)], dq_send.at[b], dq_recv.at[me], b
        )

    def part_copy(b):
        return remote(
            part_stage.at[b],
            red.at[b // parts, part],
            part_send.at[b],
            red_recv.at[b // parts, part],
            head * parts + lax.rem(b, parts),
        )

    def fin_copy(b):
        return remote(fin.at[b // parts], kv_got.at[head], fin_send.at[b // parts], fin_recv.at[head], b)

    def step(s, carry):
        b = blocks - 1 - s

        @pl.when(s < blocks)
        def _():
            compute(b)

        @pl.when((s >= 1) & (s < blocks + 1))
        def _():
            n = b + 1

            @pl.when(n == me)
            def _():
                dq_got[head, lax.rem(part + n, parts)] = dq_stage[n]

            @pl.when(n != me)
            def _():
                dq_copy(n).start()

            @pl.when(lax.rem(n, parts) != part)
            def _():
                part_copy(n).start()

        @pl.when((s >= 2) & (s < blocks + 2))
        def _():
            n = b + 2

            @pl.when(lax.rem(n, parts) == part)
            def _():
                slot = n // parts
                for c in range(1, parts):
                    other = lax.rem(part + c, parts)
                    remote(
                        red.at[slot, other], red.at[slot, other], part_send.at[0], red_recv.at[slot, other], me
                    ).wait_recv()
                for i in range(2):
                    value = dk[n] * SCALE if i == 0 else dv[n]
                    for c in range(1, parts):
                        value = value + red[slot, lax.rem(part + c, parts), i].astype(jnp.float32)
                    fin[slot, i] = value.astype(LOW)

        @pl.when(s >= 3)
        def _():
            n = b + 3

            @pl.when(lax.rem(n, parts) == part)
            def _():
                @pl.when(n == me)
                def _():
                    kv_got[head] = fin[n // parts]

                @pl.when(n != me)
                def _():
                    fin_copy(n).start()

        return carry

    lax.fori_loop(0, blocks + 3, step, 0)

    for r, c in pairs:
        h, other = place(r, c)
        slot = lax.rem(other + me, parts)
        remote(
            dq_got.at[h, slot], dq_got.at[h, slot], dq_send.at[0], dq_recv.at[h * parts + other], me
        ).wait_recv()
    for h in range(heads):
        for n in range(parts):
            piece = dq_got[h, n]
            low_out[n * sub : (n + 1) * sub, h * HEAD : (h + 1) * HEAD] = piece
            dq_out[n * sub : (n + 1) * sub, h * HEAD : (h + 1) * HEAD] = piece.astype(jnp.float32)
    for r in range(1, heads):
        h, _ = place(r, 0)
        remote(kv_got.at[h], kv_got.at[h], fin_send.at[0], fin_recv.at[h], me).wait_recv()
    for h in range(heads):
        dk_out[:, h * HEAD : (h + 1) * HEAD] = kv_got[h, 0].astype(jnp.float32)
        dv_out[:, h * HEAD : (h + 1) * HEAD] = kv_got[h, 1].astype(jnp.float32)

    for r in range(1, heads):
        for i in range(2):
            kv_copy(r, i).wait_send()
    for r in range(heads):
        for c in range(1, parts):
            for i in range(2):
                relay_copy(r, c, i).wait_send()
    for r, c in pairs:
        gate_copy(r, c).wait_send()
        for i in range(2):
            q_copy(r, c, i).wait_send()

    @pl.loop(0, blocks)
    def _(b):
        @pl.when(b != me)
        def _():
            dq_copy(b).wait_send()

        @pl.when(lax.rem(b, parts) != part)
        def _():
            part_copy(b).wait_send()

        @pl.when((lax.rem(b, parts) == part) & (b != me))
        def _():
            fin_copy(b).wait_send()


def attention(heads, parts, q, g, k, v, gate):
    blocks = heads * parts
    rows = k.shape[0]
    sub = rows // parts
    groups = blocks // parts
    vmem = pl.BlockSpec(memory_space=pltpu.VMEM)
    f32 = jnp.float32
    dma = pltpu.SemaphoreType.DMA
    wide = jax.ShapeDtypeStruct((rows, heads * HEAD), f32)
    return pl.pallas_call(
        lambda *refs: kernel_body(heads, parts, *refs),
        out_shape=(wide, jax.ShapeDtypeStruct((rows, heads * HEAD), LOW), wide, wide),
        in_specs=[vmem] * 5,
        out_specs=(vmem,) * 4,
        scratch_shapes=[
            pltpu.VMEM((blocks, 2, rows, HEAD), LOW),
            pltpu.VMEM((blocks, 2, sub, HEAD), LOW),
            pltpu.VMEM((blocks, 8, rows), f32),
            pltpu.VMEM((blocks, HEAD, rows), LOW),
            pltpu.VMEM((blocks, HEAD, rows), LOW),
            pltpu.VMEM((blocks, rows, HEAD), f32),
            pltpu.VMEM((blocks, rows, sub), f32),
            pltpu.VMEM((blocks, rows, HEAD), f32),
            pltpu.VMEM((blocks, rows, HEAD), f32),
            pltpu.VMEM((blocks, sub, HEAD), LOW),
            pltpu.VMEM((blocks, 2, rows, HEAD), LOW),
            pltpu.VMEM((groups, parts, 2, rows, HEAD), LOW),
            pltpu.VMEM((groups, 2, rows, HEAD), LOW),
            pltpu.VMEM((heads, parts, sub, HEAD), LOW),
            pltpu.VMEM((heads, 2, rows, HEAD), LOW),
            dma((blocks, 2)), dma((blocks, 2)), dma((blocks,)),
            dma((heads, 2)), dma((heads, parts, 2)), dma((heads, parts)), dma((heads, parts, 2)),
            dma((blocks,)), dma((blocks,)), dma((blocks,)), dma((groups, parts)),
            dma((groups,)), dma((heads,)), dma((5,)),
        ],
        compiler_params=pltpu.CompilerParams(
            vmem_limit_bytes=60 * 1024 * 1024, collective_id=0, has_side_effects=True
        ),
        cost_estimate=pl.CostEstimate(
            flops=12 * blocks * blocks * rows * sub * HEAD, bytes_accessed=1 << 22, transcendentals=0
        ),
        name="attention",
    )(q, g, k, v, gate)


def local(queries, keys, values, forget_logits, layer_input, out_grad):
    rows = queries.shape[0]
    heads = queries.shape[1] // HEAD
    parts = lax.axis_size("sp") // heads

    input_whole = lax.all_gather(layer_input, "tp", axis=1, tiled=True)
    gates = jnp.cumsum(jax.nn.log_sigmoid(forget_logits), axis=0).T * LOG2E
    totals = jnp.broadcast_to(gates[:, None, rows - 1 :], (heads, 7, rows))
    gates = jnp.concatenate([gates[:, None], totals], axis=1)
    query_grad, low, key_grad, value_grad = attention(
        heads, parts, queries, out_grad, keys, values, gates
    )
    weight_term = lax.dot_general(
        input_whole, low, (((0,), (0,)), ((), ())), preferred_element_type=jnp.float32
    )
    weight_grad = lax.psum_scatter(
        weight_term.astype(LOW), "sp", scatter_dimension=0, tiled=True
    ).astype(jnp.float32)
    return query_grad, key_grad, value_grad, weight_grad


def solution(mesh):
    spec = P("sp", "tp")
    return jax.shard_map(
        local, mesh=mesh, in_specs=(spec,) * 6, out_specs=(spec,) * 4, check_vma=False
    )
```

```python
import jax
import jax.numpy as jnp
from jax import lax
from jax.experimental import pallas as pl
from jax.experimental.pallas import tpu as pltpu
from jax.sharding import PartitionSpec as P

HEAD = 128
LOG2E = 1.4426950408889634
SCALE = HEAD ** (-0.5)
LOW = jnp.bfloat16


def nt(a, b):
    return lax.dot_general(a, b, (((1,), (1,)), ((), ())), preferred_element_type=jnp.float32)


def nn(a, b):
    return lax.dot_general(a, b, (((1,), (0,)), ((), ())), preferred_element_type=jnp.float32)


def kernel_body(
    heads, parts, wide,
    q_in, g_in, k_in, v_in, gate_in, x_in,
    dq_out, dk_out, dv_out, w_out,
    kv, qg, gates, kt, vt, bias, sc, dk, dv, dq_stage, part_stage, red, fin, dq_got, kv_got,
    x_all, low, w_stage, w_red, w_fin, w_got,
    kv_recv, qg_recv, gate_recv, kv_send, qg_send, gate_send, relay_send,
    dq_send, dq_recv, part_send, red_recv, fin_send, fin_recv, local_sem,
    x_send, x_recv, w_send, w_recv, w_fin_send, w_fin_recv,
):
    blocks, _, rows, _ = kv.shape
    sub = qg.shape[2]
    span = w_out.shape[0]
    x_width = x_in.shape[1]
    column = lax.axis_index("tp")
    me = lax.axis_index("sp")
    head = me // parts
    part = lax.rem(me, parts)

    def remote(src, dst, send, recv, target):
        return pltpu.make_async_remote_copy(
            src_ref=src, dst_ref=dst, send_sem=send, recv_sem=recv, device_id={"sp": target}
        )

    barrier = pltpu.get_barrier_semaphore()
    for r in range(1, blocks):
        pl.semaphore_signal(barrier, inc=1, device_id={"sp": lax.rem(me + r, blocks)})
    for r in range(1, wide):
        pl.semaphore_signal(barrier, inc=1, device_id={"tp": lax.rem(column + r, wide)})
    pl.semaphore_wait(barrier, blocks + wide - 2)

    def lanes(h):
        return pl.ds(pl.multiple_of(h * HEAD, HEAD), HEAD)

    sources = ((k_in, v_in), (q_in, g_in))

    def place(r, c):
        return lax.rem(head + r, heads), lax.rem(part + c, parts)

    def kv_copy(r, i):
        h, _ = place(r, 0)
        return remote(
            sources[0][i].at[:, lanes(h)], kv.at[me, i], kv_send.at[r, i], kv_recv.at[me, i], h * parts + part
        )

    def relay_copy(r, c, i):
        h, other = place(r, c)
        j = h * parts + part
        src = sources[0][i].at[:, lanes(head)] if r == 0 else kv.at[j, i]
        return remote(src, kv.at[j, i], relay_send.at[r, c, i], kv_recv.at[j, i], head * parts + other)

    def q_source(r, c, i):
        h, other = place(r, c)
        begin = pl.multiple_of(lax.rem(other + me, parts) * sub, sub)
        return sources[1][i].at[pl.ds(begin, sub), lanes(h)]

    def q_copy(r, c, i):
        h, other = place(r, c)
        return remote(
            q_source(r, c, i), qg.at[me, i], qg_send.at[r, c, i], qg_recv.at[me, i], h * parts + other
        )

    def gate_copy(r, c):
        h, other = place(r, c)
        return remote(gate_in.at[h], gates.at[me], gate_send.at[r, c], gate_recv.at[me], h * parts + other)

    pairs = [(r, c) for r in range(heads) for c in range(parts) if (r, c) != (0, 0)]
    for r in range(1, heads):
        for i in range(2):
            kv_copy(r, i).start()
    for c in range(1, parts):
        for i in range(2):
            relay_copy(0, c, i).start()
    for r, c in pairs:
        gate_copy(r, c).start()
        for i in range(2):
            q_copy(r, c, i).start()
    own = [
        pltpu.make_async_copy(sources[0][i].at[:, lanes(head)], kv.at[me, i], local_sem.at[i]) for i in range(2)
    ]
    own += [pltpu.make_async_copy(q_source(0, 0, i), qg.at[me, i], local_sem.at[2 + i]) for i in range(2)]
    own += [pltpu.make_async_copy(gate_in.at[head], gates.at[me], local_sem.at[4])]
    own += [pltpu.make_async_copy(x_in, x_all.at[column], local_sem.at[5])]
    for copy in own:
        copy.start()

    def x_copy(r, source):
        return pltpu.make_async_remote_copy(
            src_ref=x_in,
            dst_ref=x_all.at[source],
            send_sem=x_send.at[r],
            recv_sem=x_recv.at[source],
            device_id={"tp": lax.rem(column + r, wide)},
        )

    for r in range(1, wide):
        x_copy(r, column).start()

    def kv_wait(j):
        for i in range(2):
            remote(kv.at[j, i], kv.at[j, i], kv_send.at[0, i], kv_recv.at[j, i], me).wait_recv()

    for r in range(1, heads):
        j = place(r, 0)[0] * parts + part
        kv_wait(j)
        for c in range(1, parts):
            for i in range(2):
                relay_copy(r, c, i).start()
    for copy in own:
        copy.wait()
    for r, c in pairs:
        h, other = place(r, c)
        j = h * parts + other
        if c:
            kv_wait(j)
        for i in range(2):
            remote(qg.at[j, i], qg.at[j, i], qg_send.at[0, 0, i], qg_recv.at[j, i], me).wait_recv()
        remote(gates.at[j], gates.at[j], gate_send.at[0, 0], gate_recv.at[j], me).wait_recv()

    def prepare(j, base):
        kt[j] = kv[j, 0].T
        vt[j] = kv[j, 1].T
        row = gates[j, 0:1] + base
        bias[j] = jnp.broadcast_to(row, (HEAD, rows)).T
        dk[j] = jnp.zeros((rows, HEAD), jnp.float32)
        dv[j] = jnp.zeros((rows, HEAD), jnp.float32)
        return base + gates[j, 1:2]

    lax.fori_loop(0, blocks, prepare, jnp.zeros((1, rows), jnp.float32))

    def compute(b):
        q = qg[b, 0]
        g = qg[b, 1]
        offset = lax.rem(part + b, parts) * sub

        def score(j):
            return nt(kv[j, 0], q) * (SCALE * LOG2E) - bias[j][:, 0:1]

        def pass_a(j, top):
            s = score(j)
            sc[j] = s
            return jnp.maximum(top, jnp.max(s, axis=0, keepdims=True))

        top = lax.fori_loop(0, b, pass_a, jnp.full((1, sub), -1e30, jnp.float32))
        key_pos = lax.broadcasted_iota(jnp.int32, (rows, sub), 0)
        query_pos = lax.broadcasted_iota(jnp.int32, (rows, sub), 1) + offset
        s = jnp.where(key_pos <= query_pos, score(b), -1e30)
        sc[b] = s
        top = jnp.maximum(top, jnp.max(s, axis=0, keepdims=True))

        def pass_b(j, state):
            total, mixed = state
            w = jnp.exp2(sc[j] - top)
            sc[j] = w
            total = total + jnp.sum(w, axis=0, keepdims=True)
            return total, mixed + nn(vt[j], w.astype(LOW))

        total, mixed = lax.fori_loop(
            0, b + 1, pass_b, (jnp.zeros((1, sub), jnp.float32), jnp.zeros((HEAD, sub), jnp.float32))
        )
        attended = (mixed / total).astype(LOW).astype(jnp.float32)
        terms = jnp.sum(attended * g.astype(jnp.float32).T, axis=0, keepdims=True)
        inverse = 1.0 / total

        def pass_c(j, acc):
            prob = sc[j] * inverse
            ds = (prob * (nt(kv[j, 1], g) - terms)).astype(LOW)
            dv[j] += nn(prob.astype(LOW), g)
            dk[j] += nn(ds, q)
            return acc + nn(kt[j], ds)

        acc = lax.fori_loop(0, b + 1, pass_c, jnp.zeros((HEAD, sub), jnp.float32))
        dq_stage[b] = (acc * SCALE).T.astype(LOW)
        part_stage[b, 0] = (dk[b] * SCALE).astype(LOW)
        part_stage[b, 1] = dv[b].astype(LOW)

    def dq_copy(b):
        return remote(
            dq_stage.at[b], dq_got.at[head, lax.rem(part + b, parts)], dq_send.at[b], dq_recv.at[me], b
        )

    def part_copy(b):
        return remote(
            part_stage.at[b],
            red.at[b // parts, part],
            part_send.at[b],
            red_recv.at[b // parts, part],
            head * parts + lax.rem(b, parts),
        )

    def fin_copy(b):
        return remote(fin.at[b // parts], kv_got.at[head], fin_send.at[b // parts], fin_recv.at[head], b)

    def step(s, carry):
        b = blocks - 1 - s

        @pl.when(s < blocks)
        def _():
            compute(b)

        @pl.when((s >= 1) & (s < blocks + 1))
        def _():
            n = b + 1

            @pl.when(n == me)
            def _():
                dq_got[head, lax.rem(part + n, parts)] = dq_stage[n]

            @pl.when(n != me)
            def _():
                dq_copy(n).start()

            @pl.when(lax.rem(n, parts) != part)
            def _():
                part_copy(n).start()

        @pl.when((s >= 2) & (s < blocks + 2))
        def _():
            n = b + 2

            @pl.when(lax.rem(n, parts) == part)
            def _():
                slot = n // parts
                for c in range(1, parts):
                    other = lax.rem(part + c, parts)
                    remote(
                        red.at[slot, other], red.at[slot, other], part_send.at[0], red_recv.at[slot, other], me
                    ).wait_recv()
                for i in range(2):
                    value = dk[n] * SCALE if i == 0 else dv[n]
                    for c in range(1, parts):
                        value = value + red[slot, lax.rem(part + c, parts), i].astype(jnp.float32)
                    fin[slot, i] = value.astype(LOW)

        @pl.when(s >= 3)
        def _():
            n = b + 3

            @pl.when(lax.rem(n, parts) == part)
            def _():
                @pl.when(n == me)
                def _():
                    kv_got[head] = fin[n // parts]

                @pl.when(n != me)
                def _():
                    fin_copy(n).start()

        return carry

    lax.fori_loop(0, blocks + 3, step, 0)

    for r, c in pairs:
        h, other = place(r, c)
        slot = lax.rem(other + me, parts)
        remote(
            dq_got.at[h, slot], dq_got.at[h, slot], dq_send.at[0], dq_recv.at[h * parts + other], me
        ).wait_recv()
    for h in range(heads):
        for n in range(parts):
            low[n * sub : (n + 1) * sub, h * HEAD : (h + 1) * HEAD] = dq_got[h, n]
    for r in range(1, wide):
        x_copy(r, lax.rem(column + r, wide)).wait_recv()

    def term(c):
        begin = c * span
        x = x_all[begin // x_width, :, pl.ds(pl.multiple_of(lax.rem(begin, x_width), span), span)]
        return lax.dot_general(x, low[...], (((0,), (0,)), ((), ())), preferred_element_type=jnp.float32)

    def w_copy(r, c):
        h, other = place(r, c)
        return remote(
            w_stage.at[r, c], w_red.at[h, part], w_send.at[r, c], w_recv.at[h, part], head * parts + other
        )

    def w_fin_copy(r):
        h, _ = place(r, 0)
        return remote(w_fin.at[r], w_got.at[head], w_fin_send.at[r], w_fin_recv.at[head], h * parts + part)

    order = list(range(1, heads)) + [0]
    waiting = None
    for r in order:
        for c in range(1, parts):
            h, other = place(r, c)
            w_stage[r, c] = term(h * parts + other).astype(LOW)
            if waiting is not None:
                waiting.start()
            waiting = w_copy(r, c)
    dq_out[...] = low[...].astype(jnp.float32)
    if waiting is not None:
        waiting.start()
    waiting = None
    for r in order:
        h, _ = place(r, 0)
        w_out[...] = term(h * parts + part)
        if waiting is not None:
            waiting.start()
            waiting = None
        for c in range(1, parts):
            other = place(r, c)[1]
            remote(
                w_red.at[h, other], w_red.at[h, other], w_send.at[0, 0], w_recv.at[h, other], me
            ).wait_recv()
            w_out[...] += w_red[h, other].astype(jnp.float32)
        if r:
            w_fin[r] = w_out[...].astype(LOW)
            waiting = w_fin_copy(r)
    for r in range(1, heads):
        h, _ = place(r, 0)
        remote(kv_got.at[h], kv_got.at[h], fin_send.at[0], fin_recv.at[h], me).wait_recv()
    for h in range(heads):
        dk_out[:, h * HEAD : (h + 1) * HEAD] = kv_got[h, 0].astype(jnp.float32)
        dv_out[:, h * HEAD : (h + 1) * HEAD] = kv_got[h, 1].astype(jnp.float32)
    for r in range(1, heads):
        h, _ = place(r, 0)
        remote(w_got.at[h], w_got.at[h], w_fin_send.at[0], w_fin_recv.at[h], me).wait_recv()
        w_out[...] += w_got[h].astype(jnp.float32)
    for r in range(1, wide):
        x_copy(r, column).wait_send()
    for r in range(heads):
        for c in range(1, parts):
            w_copy(r, c).wait_send()
    for r in range(1, heads):
        w_fin_copy(r).wait_send()

    for r in range(1, heads):
        for i in range(2):
            kv_copy(r, i).wait_send()
    for r in range(heads):
        for c in range(1, parts):
            for i in range(2):
                relay_copy(r, c, i).wait_send()
    for r, c in pairs:
        gate_copy(r, c).wait_send()
        for i in range(2):
            q_copy(r, c, i).wait_send()

    @pl.loop(0, blocks)
    def _(b):
        @pl.when(b != me)
        def _():
            dq_copy(b).wait_send()

        @pl.when(lax.rem(b, parts) != part)
        def _():
            part_copy(b).wait_send()

        @pl.when((lax.rem(b, parts) == part) & (b != me))
        def _():
            fin_copy(b).wait_send()


def attention(heads, parts, wide, q, g, k, v, gate, x):
    blocks = heads * parts
    rows = k.shape[0]
    sub = rows // parts
    groups = blocks // parts
    vmem = pl.BlockSpec(memory_space=pltpu.VMEM)
    f32 = jnp.float32
    dma = pltpu.SemaphoreType.DMA
    cols = heads * HEAD
    span = x.shape[1] * wide // blocks
    grad = jax.ShapeDtypeStruct((rows, cols), f32)
    return pl.pallas_call(
        lambda *refs: kernel_body(heads, parts, wide, *refs),
        out_shape=(grad, grad, grad, jax.ShapeDtypeStruct((span, cols), f32)),
        in_specs=[vmem] * 6,
        out_specs=(vmem,) * 4,
        scratch_shapes=[
            pltpu.VMEM((blocks, 2, rows, HEAD), LOW),
            pltpu.VMEM((blocks, 2, sub, HEAD), LOW),
            pltpu.VMEM((blocks, 8, rows), f32),
            pltpu.VMEM((blocks, HEAD, rows), LOW),
            pltpu.VMEM((blocks, HEAD, rows), LOW),
            pltpu.VMEM((blocks, rows, HEAD), f32),
            pltpu.VMEM((blocks, rows, sub), f32),
            pltpu.VMEM((blocks, rows, HEAD), f32),
            pltpu.VMEM((blocks, rows, HEAD), f32),
            pltpu.VMEM((blocks, sub, HEAD), LOW),
            pltpu.VMEM((blocks, 2, rows, HEAD), LOW),
            pltpu.VMEM((groups, parts, 2, rows, HEAD), LOW),
            pltpu.VMEM((groups, 2, rows, HEAD), LOW),
            pltpu.VMEM((heads, parts, sub, HEAD), LOW),
            pltpu.VMEM((heads, 2, rows, HEAD), LOW),
            pltpu.VMEM((wide, rows, x.shape[1]), LOW),
            pltpu.VMEM((rows, cols), LOW),
            pltpu.VMEM((heads, parts, span, cols), LOW),
            pltpu.VMEM((heads, parts, span, cols), LOW),
            pltpu.VMEM((heads, span, cols), LOW),
            pltpu.VMEM((heads, span, cols), LOW),
            dma((blocks, 2)), dma((blocks, 2)), dma((blocks,)),
            dma((heads, 2)), dma((heads, parts, 2)), dma((heads, parts)), dma((heads, parts, 2)),
            dma((blocks,)), dma((blocks,)), dma((blocks,)), dma((groups, parts)),
            dma((groups,)), dma((heads,)), dma((6,)),
            dma((wide,)), dma((wide,)), dma((heads, parts)), dma((heads, parts)), dma((heads,)), dma((heads,)),
        ],
        compiler_params=pltpu.CompilerParams(
            vmem_limit_bytes=60 * 1024 * 1024, collective_id=0, has_side_effects=True
        ),
        cost_estimate=pl.CostEstimate(
            flops=12 * blocks * blocks * rows * sub * HEAD, bytes_accessed=1 << 22, transcendentals=0
        ),
        name="attention",
    )(q, g, k, v, gate, x)


def local(queries, keys, values, forget_logits, layer_input, out_grad):
    rows = queries.shape[0]
    heads = queries.shape[1] // HEAD
    parts = lax.axis_size("sp") // heads

    wide = lax.axis_size("tp")
    gates = jnp.cumsum(jax.nn.log_sigmoid(forget_logits), axis=0).T * LOG2E
    totals = jnp.broadcast_to(gates[:, None, rows - 1 :], (heads, 7, rows))
    gates = jnp.concatenate([gates[:, None], totals], axis=1)
    return attention(
        heads, parts, wide, queries, out_grad, keys, values, gates, layer_input
    )


def solution(mesh):
    spec = P("sp", "tp")
    return jax.shard_map(
        local, mesh=mesh, in_specs=(spec,) * 6, out_specs=(spec,) * 4, check_vma=False
    )
```

```python
import jax
import jax.numpy as jnp
from jax import lax
from jax.experimental import pallas as pl
from jax.experimental.pallas import tpu as pltpu
from jax.sharding import PartitionSpec as P

HEAD = 128
LOG2E = 1.4426950408889634
SCALE = HEAD ** (-0.5)
LOW = jnp.bfloat16


def nt(a, b):
    return lax.dot_general(a, b, (((1,), (1,)), ((), ())), preferred_element_type=jnp.float32)


def nn(a, b):
    return lax.dot_general(a, b, (((1,), (0,)), ((), ())), preferred_element_type=jnp.float32)


def kernel_body(
    heads, parts, wide,
    q_in, g_in, k_in, v_in, gate_in, x_in,
    dq_out, dk_out, dv_out, w_out,
    kv, qg, gates, kt, vt, bias, sc, dk, dv, dq_stage, part_stage, red, fin, dq_got, kv_got,
    x_all, low, w_stage, w_red, w_fin, w_got,
    kv_recv, qg_recv, gate_recv, kv_send, qg_send, gate_send, relay_send,
    dq_send, dq_recv, part_send, red_recv, fin_send, fin_recv, local_sem,
    x_send, x_recv, w_send, w_recv, w_fin_send, w_fin_recv,
):
    blocks, _, rows, _ = kv.shape
    sub = qg.shape[2]
    span = w_out.shape[0]
    x_width = x_in.shape[1]
    column = lax.axis_index("tp")
    me = lax.axis_index("sp")
    head = me // parts
    part = lax.rem(me, parts)

    def remote(src, dst, send, recv, target):
        return pltpu.make_async_remote_copy(
            src_ref=src, dst_ref=dst, send_sem=send, recv_sem=recv, device_id={"sp": target}
        )

    barrier = pltpu.get_barrier_semaphore()
    for r in range(1, blocks):
        pl.semaphore_signal(barrier, inc=1, device_id={"sp": lax.rem(me + r, blocks)})
    for r in range(1, wide):
        pl.semaphore_signal(barrier, inc=1, device_id={"tp": lax.rem(column + r, wide)})
    pl.semaphore_wait(barrier, blocks + wide - 2)

    def lanes(h):
        return pl.ds(pl.multiple_of(h * HEAD, HEAD), HEAD)

    sources = ((k_in, v_in), (q_in, g_in))

    def place(r, c):
        return lax.rem(head + r, heads), lax.rem(part + c, parts)

    def kv_copy(r, i):
        h, _ = place(r, 0)
        return remote(
            sources[0][i].at[:, lanes(h)], kv.at[me, i], kv_send.at[r, i], kv_recv.at[me, i], h * parts + part
        )

    def relay_copy(r, c, i):
        h, other = place(r, c)
        j = h * parts + part
        src = sources[0][i].at[:, lanes(head)] if r == 0 else kv.at[j, i]
        return remote(src, kv.at[j, i], relay_send.at[r, c, i], kv_recv.at[j, i], head * parts + other)

    def q_source(r, c, i):
        h, other = place(r, c)
        begin = pl.multiple_of(lax.rem(other + me, parts) * sub, sub)
        return sources[1][i].at[pl.ds(begin, sub), lanes(h)]

    def q_copy(r, c, i):
        h, other = place(r, c)
        return remote(
            q_source(r, c, i), qg.at[me, i], qg_send.at[r, c, i], qg_recv.at[me, i], h * parts + other
        )

    def gate_copy(r, c):
        h, other = place(r, c)
        return remote(gate_in.at[h], gates.at[me], gate_send.at[r, c], gate_recv.at[me], h * parts + other)

    pairs = [(r, c) for r in range(heads) for c in range(parts) if (r, c) != (0, 0)]
    for r in range(1, heads):
        for i in range(2):
            kv_copy(r, i).start()
    for c in range(1, parts):
        for i in range(2):
            relay_copy(0, c, i).start()
    for r, c in pairs:
        gate_copy(r, c).start()
        for i in range(2):
            q_copy(r, c, i).start()
    own = [
        pltpu.make_async_copy(sources[0][i].at[:, lanes(head)], kv.at[me, i], local_sem.at[i]) for i in range(2)
    ]
    own += [pltpu.make_async_copy(q_source(0, 0, i), qg.at[me, i], local_sem.at[2 + i]) for i in range(2)]
    own += [pltpu.make_async_copy(gate_in.at[head], gates.at[me], local_sem.at[4])]
    own += [pltpu.make_async_copy(x_in, x_all.at[column], local_sem.at[5])]
    for copy in own:
        copy.start()

    def x_copy(r, source):
        return pltpu.make_async_remote_copy(
            src_ref=x_in,
            dst_ref=x_all.at[source],
            send_sem=x_send.at[r],
            recv_sem=x_recv.at[source],
            device_id={"tp": lax.rem(column + r, wide)},
        )

    for r in range(1, wide):
        x_copy(r, column).start()

    def kv_wait(j):
        for i in range(2):
            remote(kv.at[j, i], kv.at[j, i], kv_send.at[0, i], kv_recv.at[j, i], me).wait_recv()

    def turn(j):
        kt[j] = kv[j, 0].T
        vt[j] = kv[j, 1].T

    @pl.loop(0, blocks)
    def _(j):
        dk[j] = jnp.zeros((rows, HEAD), jnp.float32)
        dv[j] = jnp.zeros((rows, HEAD), jnp.float32)

    for copy in own:
        copy.wait()
    turn(me)
    for r in range(1, heads):
        j = place(r, 0)[0] * parts + part
        kv_wait(j)
        for c in range(1, parts):
            for i in range(2):
                relay_copy(r, c, i).start()
        turn(j)
    for r, c in pairs:
        h, other = place(r, c)
        j = h * parts + other
        if c:
            kv_wait(j)
            turn(j)
        for i in range(2):
            remote(qg.at[j, i], qg.at[j, i], qg_send.at[0, 0, i], qg_recv.at[j, i], me).wait_recv()
        remote(gates.at[j], gates.at[j], gate_send.at[0, 0], gate_recv.at[j], me).wait_recv()

    def prepare(j, base):
        row = gates[j, 0:1] + base
        bias[j] = jnp.broadcast_to(row, (HEAD, rows)).T
        return base + gates[j, 1:2]

    lax.fori_loop(0, blocks, prepare, jnp.zeros((1, rows), jnp.float32))

    def compute(b):
        q = qg[b, 0]
        g = qg[b, 1]
        offset = lax.rem(part + b, parts) * sub

        def score(j):
            return nt(kv[j, 0], q) * (SCALE * LOG2E) - bias[j][:, 0:1]

        def pass_a(j, top):
            s = score(j)
            sc[j] = s
            return jnp.maximum(top, jnp.max(s, axis=0, keepdims=True))

        top = lax.fori_loop(0, b, pass_a, jnp.full((1, sub), -1e30, jnp.float32))
        key_pos = lax.broadcasted_iota(jnp.int32, (rows, sub), 0)
        query_pos = lax.broadcasted_iota(jnp.int32, (rows, sub), 1) + offset
        s = jnp.where(key_pos <= query_pos, score(b), -1e30)
        sc[b] = s
        top = jnp.maximum(top, jnp.max(s, axis=0, keepdims=True))

        def pass_b(j, state):
            total, mixed = state
            w = jnp.exp2(sc[j] - top)
            sc[j] = w
            total = total + jnp.sum(w, axis=0, keepdims=True)
            return total, mixed + nn(vt[j], w.astype(LOW))

        total, mixed = lax.fori_loop(
            0, b + 1, pass_b, (jnp.zeros((1, sub), jnp.float32), jnp.zeros((HEAD, sub), jnp.float32))
        )
        attended = (mixed / total).astype(LOW).astype(jnp.float32)
        terms = jnp.sum(attended * g.astype(jnp.float32).T, axis=0, keepdims=True)
        inverse = 1.0 / total

        def pass_c(j, acc):
            prob = sc[j] * inverse
            ds = (prob * (nt(kv[j, 1], g) - terms)).astype(LOW)
            dv[j] += nn(prob.astype(LOW), g)
            dk[j] += nn(ds, q)
            return acc + nn(kt[j], ds)

        acc = lax.fori_loop(0, b + 1, pass_c, jnp.zeros((HEAD, sub), jnp.float32))
        dq_stage[b] = (acc * SCALE).T.astype(LOW)
        part_stage[b, 0] = (dk[b] * SCALE).astype(LOW)
        part_stage[b, 1] = dv[b].astype(LOW)

    def dq_copy(b):
        return remote(
            dq_stage.at[b], dq_got.at[head, lax.rem(part + b, parts)], dq_send.at[b], dq_recv.at[me], b
        )

    def part_copy(b):
        return remote(
            part_stage.at[b],
            red.at[b // parts, part],
            part_send.at[b],
            red_recv.at[b // parts, part],
            head * parts + lax.rem(b, parts),
        )

    def fin_copy(b):
        return remote(fin.at[b // parts], kv_got.at[head], fin_send.at[b // parts], fin_recv.at[head], b)

    def step(s, carry):
        b = blocks - 1 - s

        @pl.when(s < blocks)
        def _():
            compute(b)

        @pl.when((s >= 1) & (s < blocks + 1))
        def _():
            n = b + 1

            @pl.when(n == me)
            def _():
                dq_got[head, lax.rem(part + n, parts)] = dq_stage[n]

            @pl.when(n != me)
            def _():
                dq_copy(n).start()

            @pl.when(lax.rem(n, parts) != part)
            def _():
                part_copy(n).start()

        @pl.when((s >= 2) & (s < blocks + 2))
        def _():
            n = b + 2

            @pl.when(lax.rem(n, parts) == part)
            def _():
                slot = n // parts
                for c in range(1, parts):
                    other = lax.rem(part + c, parts)
                    remote(
                        red.at[slot, other], red.at[slot, other], part_send.at[0], red_recv.at[slot, other], me
                    ).wait_recv()
                for i in range(2):
                    value = dk[n] * SCALE if i == 0 else dv[n]
                    for c in range(1, parts):
                        value = value + red[slot, lax.rem(part + c, parts), i].astype(jnp.float32)
                    fin[slot, i] = value.astype(LOW)

        @pl.when(s >= 3)
        def _():
            n = b + 3

            @pl.when(lax.rem(n, parts) == part)
            def _():
                @pl.when(n == me)
                def _():
                    kv_got[head] = fin[n // parts]

                @pl.when(n != me)
                def _():
                    fin_copy(n).start()

        return carry

    lax.fori_loop(0, blocks + 3, step, 0)

    for r, c in pairs:
        h, other = place(r, c)
        slot = lax.rem(other + me, parts)
        remote(
            dq_got.at[h, slot], dq_got.at[h, slot], dq_send.at[0], dq_recv.at[h * parts + other], me
        ).wait_recv()
    for h in range(heads):
        for n in range(parts):
            low[n * sub : (n + 1) * sub, h * HEAD : (h + 1) * HEAD] = dq_got[h, n]
    for r in range(1, wide):
        x_copy(r, lax.rem(column + r, wide)).wait_recv()

    def term(c):
        begin = c * span
        x = x_all[begin // x_width, :, pl.ds(pl.multiple_of(lax.rem(begin, x_width), span), span)]
        return lax.dot_general(x, low[...], (((0,), (0,)), ((), ())), preferred_element_type=jnp.float32)

    def w_copy(r, c):
        h, other = place(r, c)
        return remote(
            w_stage.at[r, c], w_red.at[h, part], w_send.at[r, c], w_recv.at[h, part], head * parts + other
        )

    def w_fin_copy(r):
        h, _ = place(r, 0)
        return remote(w_fin.at[r], w_got.at[head], w_fin_send.at[r], w_fin_recv.at[head], h * parts + part)

    order = list(range(1, heads)) + [0]
    waiting = None
    for r in order:
        for c in range(1, parts):
            h, other = place(r, c)
            w_stage[r, c] = term(h * parts + other).astype(LOW)
            if waiting is not None:
                waiting.start()
            waiting = w_copy(r, c)
    dq_out[...] = low[...].astype(jnp.float32)
    if waiting is not None:
        waiting.start()
    waiting = None
    for r in order:
        h, _ = place(r, 0)
        w_out[...] = term(h * parts + part)
        if waiting is not None:
            waiting.start()
            waiting = None
        for c in range(1, parts):
            other = place(r, c)[1]
            remote(
                w_red.at[h, other], w_red.at[h, other], w_send.at[0, 0], w_recv.at[h, other], me
            ).wait_recv()
            w_out[...] += w_red[h, other].astype(jnp.float32)
        if r:
            w_fin[r] = w_out[...].astype(LOW)
            waiting = w_fin_copy(r)
    for r in range(1, heads):
        h, _ = place(r, 0)
        remote(kv_got.at[h], kv_got.at[h], fin_send.at[0], fin_recv.at[h], me).wait_recv()
    for h in range(heads):
        dk_out[:, h * HEAD : (h + 1) * HEAD] = kv_got[h, 0].astype(jnp.float32)
        dv_out[:, h * HEAD : (h + 1) * HEAD] = kv_got[h, 1].astype(jnp.float32)
    for r in range(1, heads):
        h, _ = place(r, 0)
        remote(w_got.at[h], w_got.at[h], w_fin_send.at[0], w_fin_recv.at[h], me).wait_recv()
        w_out[...] += w_got[h].astype(jnp.float32)
    for r in range(1, wide):
        x_copy(r, column).wait_send()
    for r in range(heads):
        for c in range(1, parts):
            w_copy(r, c).wait_send()
    for r in range(1, heads):
        w_fin_copy(r).wait_send()

    for r in range(1, heads):
        for i in range(2):
            kv_copy(r, i).wait_send()
    for r in range(heads):
        for c in range(1, parts):
            for i in range(2):
                relay_copy(r, c, i).wait_send()
    for r, c in pairs:
        gate_copy(r, c).wait_send()
        for i in range(2):
            q_copy(r, c, i).wait_send()

    @pl.loop(0, blocks)
    def _(b):
        @pl.when(b != me)
        def _():
            dq_copy(b).wait_send()

        @pl.when(lax.rem(b, parts) != part)
        def _():
            part_copy(b).wait_send()

        @pl.when((lax.rem(b, parts) == part) & (b != me))
        def _():
            fin_copy(b).wait_send()


def attention(heads, parts, wide, q, g, k, v, gate, x):
    blocks = heads * parts
    rows = k.shape[0]
    sub = rows // parts
    groups = blocks // parts
    vmem = pl.BlockSpec(memory_space=pltpu.VMEM)
    f32 = jnp.float32
    dma = pltpu.SemaphoreType.DMA
    cols = heads * HEAD
    span = x.shape[1] * wide // blocks
    grad = jax.ShapeDtypeStruct((rows, cols), f32)
    return pl.pallas_call(
        lambda *refs: kernel_body(heads, parts, wide, *refs),
        out_shape=(grad, grad, grad, jax.ShapeDtypeStruct((span, cols), f32)),
        in_specs=[vmem] * 6,
        out_specs=(vmem,) * 4,
        scratch_shapes=[
            pltpu.VMEM((blocks, 2, rows, HEAD), LOW),
            pltpu.VMEM((blocks, 2, sub, HEAD), LOW),
            pltpu.VMEM((blocks, 8, rows), f32),
            pltpu.VMEM((blocks, HEAD, rows), LOW),
            pltpu.VMEM((blocks, HEAD, rows), LOW),
            pltpu.VMEM((blocks, rows, HEAD), f32),
            pltpu.VMEM((blocks, rows, sub), f32),
            pltpu.VMEM((blocks, rows, HEAD), f32),
            pltpu.VMEM((blocks, rows, HEAD), f32),
            pltpu.VMEM((blocks, sub, HEAD), LOW),
            pltpu.VMEM((blocks, 2, rows, HEAD), LOW),
            pltpu.VMEM((groups, parts, 2, rows, HEAD), LOW),
            pltpu.VMEM((groups, 2, rows, HEAD), LOW),
            pltpu.VMEM((heads, parts, sub, HEAD), LOW),
            pltpu.VMEM((heads, 2, rows, HEAD), LOW),
            pltpu.VMEM((wide, rows, x.shape[1]), LOW),
            pltpu.VMEM((rows, cols), LOW),
            pltpu.VMEM((heads, parts, span, cols), LOW),
            pltpu.VMEM((heads, parts, span, cols), LOW),
            pltpu.VMEM((heads, span, cols), LOW),
            pltpu.VMEM((heads, span, cols), LOW),
            dma((blocks, 2)), dma((blocks, 2)), dma((blocks,)),
            dma((heads, 2)), dma((heads, parts, 2)), dma((heads, parts)), dma((heads, parts, 2)),
            dma((blocks,)), dma((blocks,)), dma((blocks,)), dma((groups, parts)),
            dma((groups,)), dma((heads,)), dma((6,)),
            dma((wide,)), dma((wide,)), dma((heads, parts)), dma((heads, parts)), dma((heads,)), dma((heads,)),
        ],
        compiler_params=pltpu.CompilerParams(
            vmem_limit_bytes=60 * 1024 * 1024, collective_id=0, has_side_effects=True
        ),
        cost_estimate=pl.CostEstimate(
            flops=12 * blocks * blocks * rows * sub * HEAD, bytes_accessed=1 << 22, transcendentals=0
        ),
        name="attention",
    )(q, g, k, v, gate, x)


def local(queries, keys, values, forget_logits, layer_input, out_grad):
    rows = queries.shape[0]
    heads = queries.shape[1] // HEAD
    parts = lax.axis_size("sp") // heads

    wide = lax.axis_size("tp")
    gates = jnp.cumsum(jax.nn.log_sigmoid(forget_logits), axis=0).T * LOG2E
    totals = jnp.broadcast_to(gates[:, None, rows - 1 :], (heads, 7, rows))
    gates = jnp.concatenate([gates[:, None], totals], axis=1)
    return attention(
        heads, parts, wide, queries, out_grad, keys, values, gates, layer_input
    )


def solution(mesh):
    spec = P("sp", "tp")
    return jax.shard_map(
        local, mesh=mesh, in_specs=(spec,) * 6, out_specs=(spec,) * 4, check_vma=False
    )
```
